32 devices in a mesh: sp: 8 (over z, x), tp: 4 (over y, core).
Axes of the slice: x: 2, y: 2, z: 4, core: 2. Of those that a mesh axis runs over, the one named last changes fastest.
Arguments:
- inputs: bfloat16 [4096, 2048], P(('sp', 'tp')), may hold values from -6 to 6
- norm_gain: float32 [2048], replicated, may hold values from 0.1 to 1.9
- w_query: bfloat16 [2048, 1024], P(None, 'tp'), may hold values from -1 to 1
- w_key: bfloat16 [2048, 1024], P(None, 'tp'), may hold values from -1 to 1
- w_value: bfloat16 [2048, 1024], P(None, 'tp'), may hold values from -0.125 to 0.125
- query_gain: float32 [2, 64], replicated, may hold values from 1 to 5.5
- key_gain: float32 [2, 64], replicated, may hold values from 1 to 5.5
- lambdas: float32 [8], P('tp'), may hold values from 0.3 to 0.8
- sub_gain: float32 [128], replicated, may hold values from 0.1 to 1.9
- w_gate_b: bfloat16 [2048, 1024], P(None, 'tp'), may hold values from -0.125 to 0.125
- w_gate_c: bfloat16 [2048, 1024], P(None, 'tp'), may hold values from -0.125 to 0.125
- w_conv_in: bfloat16 [2048, 1024], P(None, 'tp'), may hold values from -0.125 to 0.125
- conv_taps: float32 [3, 1024], P(None, 'tp'), may hold values from -3 to 3
- conv_gain: float32 [1024], P('tp'), may hold values from 0.1 to 1.9
- w_out_att: bfloat16 [1024, 2048], P('tp'), may hold values from -0.125 to 0.125
- w_out_conv: bfloat16 [1024, 2048], P('tp'), may hold values from -0.125 to 0.125
Outputs:
- mixed: float32 [4096, 2048], P(('sp', 'tp'))
- log_sums: float32 [8, 2, 4096], P('tp', None, 'sp')
The draws below stay inside these ranges and needn't reach their ends.
All inputs are finite; a program needn't handle non-finite values.
Results may differ from the reference program's by a relative error of at most 0.034.
Values may be sent and summed in bfloat16 or wider, within the bound.
A program may use at most 192 MiB of HBM per device.

```python
import math
import jax
import jax.numpy as jnp
from jax import lax

D = 2048
ATT_HEADS = 8
QK = 64
VD = 128
CONV = 1024
GROUP = 64
KW = 3
TOKENS = 4096


def draw_query_gain(key, part):
    spread = jax.random.uniform(jax.random.fold_in(key, 11), (2, QK), jnp.float32, -1.0, 1.0)
    return 1.3 * (1.0 + 0.2 * spread)


def draw_key_gain(key, part):
    spread = jax.random.uniform(jax.random.fold_in(key, 23), (2, QK), jnp.float32, -1.0, 1.0)
    return 1.3 * (1.0 + 0.2 * spread)


def projection_pair(key):
    first = jax.random.normal(jax.random.fold_in(key, 101), (D, ATT_HEADS * 2 * QK), jnp.float32)
    second = jax.random.normal(jax.random.fold_in(key, 103), (D, ATT_HEADS * 2 * QK), jnp.float32)
    scale = D ** (-0.5)
    return (jnp.clip(first, -5.0, 5.0) * scale, jnp.clip(second, -5.0, 5.0) * scale)


def draw_w_query(key, part):
    first, second = projection_pair(key)
    return first.astype(jnp.bfloat16)


def draw_w_key(key, part):
    first, second = projection_pair(key)
    return second.astype(jnp.bfloat16)


def draw_inputs(key, part):
    base = jax.random.normal(jax.random.fold_in(key, 201), (TOKENS, D), jnp.float32)
    return jnp.clip(base, -6.0, 6.0).astype(jnp.bfloat16)


def block_levels(own_key, shape, pieces, low, high):
    loudness = 1.0
    for dim, shards_of in pieces:
        draws = jax.random.uniform(jax.random.fold_in(jax.random.fold_in(own_key, 6), dim), (shards_of,), jnp.float32, low / len(pieces), high / len(pieces))
        loudness = loudness * jnp.repeat(jnp.exp(draws), shape[dim] // shards_of).reshape((-1,) + (1,) * (len(shape) - 1 - dim))
    return loudness


def scatter_about(key, shape, deviation, reach, cuts=(), held_as=jnp.bfloat16):
    array = jax.random.normal(key, shape, jnp.float32) * deviation
    if len(cuts) > 0:
        array = block_levels(key, shape, cuts, -0.22, 0.18) * array
    return jnp.clip(array, min=-reach, max=reach).astype(held_as)


def setup_inputs(seed: int = 0) -> dict:
    key_list = jax.random.split(jax.random.key(seed), 17)
    inputs = draw_inputs(jax.random.fold_in(key_list[16], 71), 0)
    norm_gain = jnp.clip(1.0 + 0.18 * jax.random.normal(key_list[1], (D,), jnp.float32), 0.1, 1.9)
    w_query = draw_w_query(jax.random.fold_in(key_list[16], 71), 0)
    w_key = draw_w_key(jax.random.fold_in(key_list[16], 71), 0)
    w_value = scatter_about(key_list[4], (D, ATT_HEADS * VD), D ** -0.5, 0.125, ((1, 4),))
    query_gain = draw_query_gain(jax.random.fold_in(key_list[16], 71), 0)
    key_gain = draw_key_gain(jax.random.fold_in(key_list[16], 71), 0)
    lambdas = jnp.clip(0.3 + 0.5 * jax.random.uniform(key_list[7], (ATT_HEADS,), jnp.float32) ** block_levels(key_list[7], (ATT_HEADS,), ((0, 4),), -0.2, 0.2), 0.3, 0.8)
    sub_gain = jnp.clip(1.0 + 0.18 * jax.random.normal(key_list[8], (VD,), jnp.float32), 0.1, 1.9)
    w_gate_b = scatter_about(key_list[9], (D, CONV), D ** -0.5, 0.125, ((1, 4),))
    w_gate_c = scatter_about(key_list[10], (D, CONV), D ** -0.5, 0.125, ((1, 4),))
    w_conv_in = scatter_about(key_list[11], (D, CONV), D ** -0.5, 0.125, ((1, 4),))
    conv_taps = scatter_about(key_list[12], (KW, CONV), 0.577, 3.0, ((1, 4),), jnp.float32)
    conv_gain = jnp.clip(1.0 + 0.18 * jax.random.normal(key_list[13], (CONV,), jnp.float32), 0.1, 1.9)
    w_out_att = scatter_about(key_list[14], (ATT_HEADS * VD, D), (ATT_HEADS * VD + CONV) ** -0.5, 0.125, ((0, 4),))
    w_out_conv = scatter_about(key_list[15], (CONV, D), (ATT_HEADS * VD + CONV) ** -0.5, 0.125, ((0, 4),))
    return {"inputs": inputs, "norm_gain": norm_gain, "w_query": w_query, "w_key": w_key, "w_value": w_value, "query_gain": query_gain, "key_gain": key_gain, "lambdas": lambdas, "sub_gain": sub_gain, "w_gate_b": w_gate_b, "w_gate_c": w_gate_c, "w_conv_in": w_conv_in, "conv_taps": conv_taps, "conv_gain": conv_gain, "w_out_att": w_out_att, "w_out_conv": w_out_conv}


eps = 1e-06

def rms_scale(values):
    return values * lax.rsqrt(lax.optimization_barrier(jnp.mean(values * values, axis=-1, keepdims=True)) + eps)

def rounded(values):
    return lax.optimization_barrier(values.astype(jnp.bfloat16)).astype(jnp.float32)

def reference(inputs, norm_gain, w_query, w_key, w_value, query_gain, key_gain, lambdas, sub_gain, w_gate_b, w_gate_c, w_conv_in, conv_taps, conv_gain, w_out_att, w_out_conv):
    length = inputs.shape[0]
    normed = (rms_scale(inputs.astype(jnp.float32)) * norm_gain).astype(jnp.bfloat16)

    def project(weight):
        return jnp.dot(normed, weight, preferred_element_type=jnp.float32).astype(jnp.bfloat16)
    query = project(w_query).reshape(length, ATT_HEADS, 2, QK)
    key = project(w_key).reshape(length, ATT_HEADS, 2, QK)
    value = project(w_value).reshape(length, ATT_HEADS, VD)
    qn = (rms_scale(query.astype(jnp.float32)) * query_gain * QK ** (-0.5)).astype(jnp.bfloat16)
    kn = (rms_scale(key.astype(jnp.float32)) * key_gain).astype(jnp.bfloat16)
    keys_f = kn.astype(jnp.float32)
    values_f = value.astype(jnp.float32)
    qblock = math.gcd(length, 128)
    key_pos = jnp.arange(length, dtype=jnp.int32)

    def one_block(start):
        qrows = lax.dynamic_slice_in_dim(qn, start, qblock, 0).astype(jnp.float32)
        scores = jnp.einsum('qhmd,khmd->hmqk', qrows, keys_f)
        query_pos = start + jnp.arange(qblock, dtype=jnp.int32)
        allowed = key_pos[None, :] <= query_pos[:, None]
        scores = jnp.where(allowed, scores, -1e+30)
        top = lax.optimization_barrier(jnp.max(scores, axis=-1, keepdims=True))
        prob = jnp.where(allowed, jnp.exp(scores - top), 0.0)
        total = lax.optimization_barrier(jnp.sum(prob, axis=-1))
        acc = jnp.einsum('hmqk,khd->hmqd', rounded(prob), values_f)
        return (acc / total[..., None], top[..., 0] + jnp.log(total))
    starts = (jnp.arange(length // qblock) * qblock).astype(jnp.int32)
    outs, logs = lax.map(one_block, starts)
    map_out = outs.transpose(1, 2, 0, 3, 4).reshape(ATT_HEADS, 2, length, VD)
    attn = map_out[:, 0] - lambdas[:, None, None] * map_out[:, 1]
    heads_out = (rms_scale(attn) * sub_gain).astype(jnp.bfloat16)
    heads_out = heads_out.transpose(1, 0, 2).reshape(length, ATT_HEADS * VD)
    log_sums = logs.transpose(1, 2, 0, 3).reshape(ATT_HEADS, 2, length)
    gate_b = project(w_gate_b).astype(jnp.float32)
    gate_c = project(w_gate_c).astype(jnp.float32)
    conv_in = project(w_conv_in).astype(jnp.float32)
    u_vals = rounded(gate_c * conv_in)
    padded = jnp.concatenate([jnp.zeros((KW - 1, CONV), jnp.float32), u_vals], axis=0)
    conv = jnp.zeros((length, CONV), jnp.float32)
    for tap in range(KW):
        conv = conv + conv_taps[tap] * padded[tap:tap + length]
    gated = gate_b * conv
    grouped = rms_scale(gated.reshape(length, CONV // GROUP, GROUP)).reshape(length, CONV)
    conv_out = (grouped * conv_gain).astype(jnp.bfloat16)
    mixed = jnp.dot(heads_out, w_out_att, preferred_element_type=jnp.float32)
    mixed = mixed + jnp.dot(conv_out, w_out_conv, preferred_element_type=jnp.float32)
    return (mixed, log_sums)
```

```python
import functools

import jax
import jax.numpy as jnp
from jax import lax
from jax.experimental import pallas as pl
from jax.experimental.pallas import tpu as pltpu
from jax.sharding import PartitionSpec as P

GROUP = 64
eps = 1e-06
MESH = pl.DeviceIdType.MESH
VMEM_LIMIT = 60 * 1024 * 1024


def from_behind(shard, axis, by):
    count = lax.axis_size(axis)
    pairs = [(i, i + by) for i in range(count) if 0 <= i + by < count]
    return lax.ppermute(shard, axis, pairs)


def rms_scale(values):
    return values * lax.rsqrt(jnp.mean(values * values, axis=-1, keepdims=True) + eps)


def flip(index, bit):
    return index + bit - 2 * bit * lax.rem(index // bit, 2)


def remote(src, dst, send, recv, axis, target):
    return pltpu.make_async_remote_copy(
        src_ref=src,
        dst_ref=dst,
        send_sem=send,
        recv_sem=recv,
        device_id={axis: target},
        device_id_type=MESH,
    )


def greet(axis, targets):
    barrier = pltpu.get_barrier_semaphore()
    for target in targets:
        pl.semaphore_signal(barrier, inc=1, device_id={axis: target}, device_id_type=MESH)
    pl.semaphore_wait(barrier, len(targets))


CHUNKS = 4


def gather_project(x_ref, gain_ref, *rest):
    weights = rest[:6]
    att_ref, conv_ref, held, wbuf = rest[6:10]
    wsem, far_send, far_recv, near_sem, fwd_send, fwd_recv = rest[10:]
    me = lax.axis_index("tp")
    near, far = flip(me, 1), flip(me, 2)
    diag = flip(near, 2)
    rows = x_ref.shape[0]
    wcols = wbuf.shape[2]
    loads = [pltpu.make_async_copy(w, wbuf.at[i], wsem.at[i]) for i, w in enumerate(weights)]
    for load in loads:
        load.start()
    x = x_ref[...].astype(jnp.float32)
    held[me] = (rms_scale(x) * gain_ref[...]).astype(jnp.bfloat16)
    greet("tp", (near, far))
    part = rows // CHUNKS

    def far_copy(c):
        spot = held.at[me, pl.ds(c * part, part)]
        return remote(spot, spot, far_send.at[c], far_recv.at[c], "tp", far)

    def forward(c):
        spot = held.at[far, pl.ds(c * part, part)]
        return remote(spot, spot, fwd_send.at[c], fwd_recv.at[c], "tp", near)

    far_copies = [far_copy(c) for c in range(CHUNKS)]
    forwards = [forward(c) for c in range(CHUNKS)]
    near_copy = remote(held.at[me], held.at[me], near_sem.at[0], near_sem.at[1], "tp", near)
    for copy in far_copies:
        copy.start()
    near_copy.start()

    def project(slot):
        block = held[slot]
        at = pl.ds(pl.multiple_of(slot * rows, rows), rows)
        for i in range(6):
            out = att_ref if i < 3 else conv_ref
            out[at, (i % 3) * wcols : (i % 3 + 1) * wcols] = jnp.dot(
                block, wbuf[i], preferred_element_type=jnp.float32
            ).astype(jnp.bfloat16)

    for load in loads:
        load.wait()
    project(me)
    near_copy.wait_recv()
    project(near)
    for c in range(CHUNKS):
        far_copies[c].wait_recv()
        forwards[c].start()
    project(far)
    for copy in forwards:
        copy.wait_recv()
    project(diag)
    near_copy.wait_send()
    for copy in far_copies + forwards:
        copy.wait_send()


def attend(
    heads, q_ref, kv_ref, lam_ref, sub_ref, out_ref, log_ref, buf, qpad, top, total, acc,
    up_send, side_send, recv,
):
    n = buf.shape[0]
    me = lax.axis_index("sp")
    z, x = me // 2, lax.rem(me, 2)
    levels = n // 2
    partner = z * 2 + 1 - x
    rows = q_ref.shape[0]
    both = q_ref.shape[1] // heads
    comp = both // 2
    vsize = sub_ref.shape[0]
    barrier = pltpu.get_barrier_semaphore()
    has_up, has_down = z < levels - 1, z > 0
    pl.semaphore_signal(barrier, inc=1, device_id={"sp": partner}, device_id_type=MESH)

    @pl.when(has_up)
    def _():
        pl.semaphore_signal(barrier, inc=1, device_id={"sp": me + 2}, device_id_type=MESH)

    @pl.when(has_down)
    def _():
        pl.semaphore_signal(barrier, inc=1, device_id={"sp": me - 2}, device_id_type=MESH)

    pl.semaphore_wait(barrier, 1 + has_up.astype(jnp.int32) + has_down.astype(jnp.int32))

    def up_copy(src, block):
        return remote(
            src, buf.at[block], up_send.at[block // 2], recv.at[block], "sp",
            jnp.minimum(me + 2, n - 2 + x),
        )

    def side_copy(src, block):
        return remote(
            src, buf.at[block], side_send.at[block // 2], recv.at[block], "sp", partner
        )

    @pl.when(has_up)
    def _():
        up_copy(kv_ref, me).start()

    @pl.when(x == 0)
    def _():
        side_copy(kv_ref, me).start()

    lane = lax.broadcasted_iota(jnp.int32, (rows, both), 1)
    for h in range(heads):
        q = q_ref[:, h * both : (h + 1) * both]
        zero = jnp.zeros_like(q)
        qpad[h, :rows] = jnp.where(lane < comp, q, zero)
        qpad[h, rows:] = jnp.where(lane < comp, zero, q)
    top[...] = jnp.full_like(top, -1e30)
    total[...] = jnp.zeros_like(total)
    acc[...] = jnp.zeros_like(acc)
    tile = min(256, rows)

    def absorb(piece, masked):
        for h in range(heads):
            for start in range(0, 2 * rows, tile):
                first = start % rows
                keys = first + tile if masked else rows
                k = piece[:keys, h * both : (h + 1) * both]
                v = piece[:keys, heads * both + h * vsize : heads * both + (h + 1) * vsize]
                at = slice(start, start + tile)
                s = lax.dot_general(
                    k, qpad[h, at], (((1,), (1,)), ((), ())), preferred_element_type=jnp.float32
                )
                if masked:
                    kpos = lax.broadcasted_iota(jnp.int32, s.shape, 0)
                    qpos = first + lax.broadcasted_iota(jnp.int32, s.shape, 1)
                    s = jnp.where(kpos <= qpos, s, -1e30)
                old = top[h : h + 1, at]
                new = jnp.maximum(old, jnp.max(s, axis=0, keepdims=True))
                p = jnp.exp(s - new)
                factor = jnp.exp(old - new)
                top[h : h + 1, at] = new
                total[h : h + 1, at] = total[h : h + 1, at] * factor + jnp.sum(
                    p, axis=0, keepdims=True
                )
                acc[h, :, at] = acc[h, :, at] * factor + lax.dot_general(
                    v, p.astype(jnp.bfloat16), (((0,), (0,)), ((), ())),
                    preferred_element_type=jnp.float32,
                )

    absorb(kv_ref, True)

    @pl.loop(0, 2 * (z + 1))
    def _(j):
        step, other = j // 2 + 1, lax.rem(j, 2)
        level = z - step + other
        block = jnp.maximum(level, 0) * 2 + x + other * (1 - 2 * x)
        valid = jnp.where(other == 0, step <= z, (x == 1) | (step >= 2))

        @pl.when(valid)
        def _():
            side_copy(buf.at[block], block).wait_recv()

            @pl.when(other == 0)
            def _():
                @pl.when(has_up)
                def _():
                    up_copy(buf.at[block], block).start()

                side_copy(buf.at[block], block).start()

            absorb(buf.at[block], False)

    for h in range(heads):
        mapped = acc[h] / total[h : h + 1]
        attn = mapped[:, :rows] - lam_ref[h] * mapped[:, rows:]
        scale = lax.rsqrt(jnp.mean(attn * attn, axis=0, keepdims=True) + eps)
        result = attn * scale * sub_ref[...]
        out_ref[:, h * vsize : (h + 1) * vsize] = result.T.astype(jnp.bfloat16)
    log_ref[...] = top[...] + jnp.log(total[...])

    @pl.loop(0, z + 1)
    def _(level):
        block = level * 2 + x

        @pl.when(has_up)
        def _():
            up_copy(kv_ref, block).wait_send()

        @pl.when((x == 0) | (level < z))
        def _():
            side_copy(kv_ref, block).wait_send()


def project_scatter(
    heads_ref, conv_ref, wa_ref, wc_ref, out_ref, cross, fin, far, cross_in, fin_in, far_in,
    cross_send, cross_recv, fin_send, fin_recv, far_send, far_recv,
):
    me = lax.axis_index("tp")
    near, other = flip(me, 1), flip(me, 2)
    diag = flip(near, 2)
    rows = out_ref.shape[0]
    width = out_ref.shape[1] // CHUNKS
    greet("tp", (near, other))

    def partial(target, c):
        at = pl.ds(pl.multiple_of(target * rows, rows), rows)
        cols = slice(c * width, (c + 1) * width)
        return jnp.dot(
            heads_ref[at, :], wa_ref[:, cols], preferred_element_type=jnp.float32
        ) + jnp.dot(conv_ref[at, :], wc_ref[:, cols], preferred_element_type=jnp.float32)

    crosses = [
        remote(cross.at[c], cross_in.at[c], cross_send.at[c], cross_recv.at[c], "tp", near)
        for c in range(CHUNKS)
    ]
    fins = [
        remote(fin.at[c], fin_in.at[c], fin_send.at[c], fin_recv.at[c], "tp", near)
        for c in range(CHUNKS)
    ]
    fars = [
        remote(far.at[c], far_in.at[c], far_send.at[c], far_recv.at[c], "tp", other)
        for c in range(CHUNKS)
    ]
    for c in range(CHUNKS):
        cross[c] = partial(diag, c).astype(jnp.bfloat16)
        crosses[c].start()
    for c in range(CHUNKS):
        mine = partial(other, c)
        crosses[c].wait_recv()
        far[c] = (mine + cross_in[c].astype(jnp.float32)).astype(jnp.bfloat16)
        fars[c].start()
    for c in range(CHUNKS):
        fin[c] = partial(near, c).astype(jnp.bfloat16)
        fins[c].start()
    for c in range(CHUNKS):
        cols = slice(c * width, (c + 1) * width)
        out_ref[:, cols] = partial(me, c)
    for c in range(CHUNKS):
        cols = slice(c * width, (c + 1) * width)
        fins[c].wait_recv()
        fars[c].wait_recv()
        out_ref[:, cols] += fin_in[c].astype(jnp.float32) + far_in[c].astype(jnp.float32)
    for copy in crosses + fins + fars:
        copy.wait_send()


def vmem():
    return pl.BlockSpec(memory_space=pltpu.VMEM)


def on_device(
    inputs, norm_gain, w_query, w_key, w_value, query_gain, key_gain, lambdas, sub_gain,
    w_gate_b, w_gate_c, w_conv_in, conv_taps, conv_gain, w_out_att, w_out_conv,
):
    heads = lambdas.shape[0]
    comp = query_gain.shape[1]
    vsize = sub_gain.shape[0]
    channels = conv_gain.shape[0]
    taps_count = conv_taps.shape[0]
    own, width = inputs.shape
    tp = lax.axis_size("tp")
    sp = lax.axis_size("sp")
    rows = own * tp
    dma = pltpu.SemaphoreType.DMA

    def params(cid):
        return pltpu.CompilerParams(
            collective_id=cid, has_side_effects=True, vmem_limit_bytes=VMEM_LIMIT
        )

    qcols = heads * 2 * comp
    weights = (w_query, w_key, w_value, w_gate_b, w_gate_c, w_conv_in)
    att_proj, conv_proj = pl.pallas_call(
        gather_project,
        out_shape=(
            jax.ShapeDtypeStruct((rows, 3 * qcols), jnp.bfloat16),
            jax.ShapeDtypeStruct((rows, 3 * channels), jnp.bfloat16),
        ),
        in_specs=[vmem(), vmem()] + [pl.BlockSpec(memory_space=pl.ANY)] * 6,
        out_specs=(vmem(), vmem()),
        scratch_shapes=[
            pltpu.VMEM((tp, own, width), jnp.bfloat16),
            pltpu.VMEM((6, width, qcols), jnp.bfloat16),
            dma((6,)), dma((CHUNKS,)), dma((CHUNKS,)), dma((2,)), dma((CHUNKS,)), dma((CHUNKS,)),
        ],
        compiler_params=params(0),
        name="gather_project",
    )(inputs, norm_gain[None], *weights)

    query = att_proj[:, :qcols].reshape(rows, heads, 2, comp)
    key = att_proj[:, qcols : 2 * qcols].reshape(rows, heads, 2, comp)
    value = att_proj[:, 2 * qcols :]
    qn = (rms_scale(query.astype(jnp.float32)) * query_gain * comp ** (-0.5)).astype(jnp.bfloat16)
    kn = (rms_scale(key.astype(jnp.float32)) * key_gain).astype(jnp.bfloat16)
    kv = jnp.concatenate([kn.reshape(rows, qcols), value], axis=1)
    heads_out, logs = pl.pallas_call(
        functools.partial(attend, heads),
        out_shape=(
            jax.ShapeDtypeStruct((rows, heads * vsize), jnp.bfloat16),
            jax.ShapeDtypeStruct((heads, 2 * rows), jnp.float32),
        ),
        in_specs=[vmem(), vmem(), pl.BlockSpec(memory_space=pltpu.SMEM), vmem()],
        out_specs=(vmem(), vmem()),
        scratch_shapes=[
            pltpu.VMEM((sp, rows, kv.shape[1]), jnp.bfloat16),
            pltpu.VMEM((heads, 2 * rows, 2 * comp), jnp.bfloat16),
            pltpu.VMEM((heads, 2 * rows), jnp.float32),
            pltpu.VMEM((heads, 2 * rows), jnp.float32),
            pltpu.VMEM((heads, vsize, 2 * rows), jnp.float32),
            dma((sp // 2,)), dma((sp // 2,)), dma((sp,)),
        ],
        compiler_params=params(1),
        cost_estimate=pl.CostEstimate(flops=20_000_000_000, bytes_accessed=0, transcendentals=0),
        name="attend",
    )(qn.reshape(rows, qcols), kv, lambdas, sub_gain[:, None])
    log_sums = logs.reshape(heads, 2, rows)

    gate_b = conv_proj[:, :channels].astype(jnp.float32)
    gate_c = conv_proj[:, channels : 2 * channels].astype(jnp.float32)
    conv_in = conv_proj[:, 2 * channels :].astype(jnp.float32)
    u_vals = (gate_c * conv_in).astype(jnp.bfloat16)
    edge = from_behind(u_vals[rows - (taps_count - 1) :], "sp", 1)
    padded = jnp.concatenate([edge, u_vals], axis=0).astype(jnp.float32)
    conv = conv_taps[0] * padded[0:rows]
    for tap in range(1, taps_count):
        conv = conv + conv_taps[tap] * padded[tap : tap + rows]
    gated = gate_b * conv
    grouped = rms_scale(gated.reshape(rows, channels // GROUP, GROUP)).reshape(rows, channels)
    conv_out = (grouped * conv_gain).astype(jnp.bfloat16)

    piece = pltpu.VMEM((CHUNKS, own, width // CHUNKS), jnp.bfloat16)
    mixed = pl.pallas_call(
        project_scatter,
        out_shape=jax.ShapeDtypeStruct((own, width), jnp.float32),
        in_specs=[vmem()] * 4,
        out_specs=vmem(),
        scratch_shapes=[piece] * 6 + [dma((CHUNKS,))] * 6,
        compiler_params=params(2),
        name="project_scatter",
    )(heads_out, conv_out, w_out_att, w_out_conv)
    return (mixed, log_sums)


def solution(mesh):
    in_specs = (
        P(("sp", "tp"), None),
        P(),
        P(None, "tp"),
        P(None, "tp"),
        P(None, "tp"),
        P(),
        P(),
        P("tp"),
        P(),
        P(None, "tp"),
        P(None, "tp"),
        P(None, "tp"),
        P(None, "tp"),
        P("tp"),
        P("tp", None),
        P("tp", None),
    )
    out_specs = (P(("sp", "tp"), None), P("tp", None, "sp"))
    return jax.shard_map(
        on_device, mesh=mesh, in_specs=in_specs, out_specs=out_specs, check_vma=False
    )
```

```python
import functools

import jax
import jax.numpy as jnp
from jax import lax
from jax.experimental import pallas as pl
from jax.experimental.pallas import tpu as pltpu
from jax.sharding import PartitionSpec as P

GROUP = 64
eps = 1e-06
MESH = pl.DeviceIdType.MESH
VMEM_LIMIT = 60 * 1024 * 1024


def rms_scale(values):
    return values * lax.rsqrt(jnp.mean(values * values, axis=-1, keepdims=True) + eps)


def flip(index, bit):
    return index + bit - 2 * bit * lax.rem(index // bit, 2)


def remote(src, dst, send, recv, axis, target):
    return pltpu.make_async_remote_copy(
        src_ref=src,
        dst_ref=dst,
        send_sem=send,
        recv_sem=recv,
        device_id={axis: target},
        device_id_type=MESH,
    )


def greet(axis, targets):
    barrier = pltpu.get_barrier_semaphore()
    for target in targets:
        pl.semaphore_signal(barrier, inc=1, device_id={axis: target}, device_id_type=MESH)
    pl.semaphore_wait(barrier, len(targets))


CHUNKS = 4
HALVES = 2


def group_scale(values, size):
    lanes = values.shape[1]
    row = lax.broadcasted_iota(jnp.int32, (lanes, lanes), 0) // size
    col = lax.broadcasted_iota(jnp.int32, (lanes, lanes), 1) // size
    ones = jnp.where(row == col, 1.0, 0.0).astype(jnp.bfloat16)
    squares = values * values
    high = squares.astype(jnp.bfloat16)
    low = (squares - high.astype(jnp.float32)).astype(jnp.bfloat16)
    sums = jnp.dot(high, ones, preferred_element_type=jnp.float32) + jnp.dot(
        low, ones, preferred_element_type=jnp.float32
    )
    return lax.rsqrt(sums * (1.0 / size) + eps)


def gather_project(comp, x_ref, gain_ref, qk_ref, *rest):
    weights = rest[:6]
    q_ref, kv_ref, conv_ref, held, wbuf = rest[6:11]
    wsem, far_send, far_recv, near_sem, fwd_send, fwd_recv = rest[11:]
    me = lax.axis_index("tp")
    near, far = flip(me, 1), flip(me, 2)
    diag = flip(near, 2)
    rows = x_ref.shape[0]
    wcols = wbuf.shape[2]
    loads = [pltpu.make_async_copy(w, wbuf.at[i], wsem.at[i]) for i, w in enumerate(weights)]
    for load in loads:
        load.start()
    x = x_ref[...].astype(jnp.float32)
    held[me] = (rms_scale(x) * gain_ref[...]).astype(jnp.bfloat16)
    greet("tp", (near, far))
    part = rows // CHUNKS

    def far_copy(c):
        spot = held.at[me, pl.ds(c * part, part)]
        return remote(spot, spot, far_send.at[c], far_recv.at[c], "tp", far)

    def forward(c):
        spot = held.at[far, pl.ds(c * part, part)]
        return remote(spot, spot, fwd_send.at[c], fwd_recv.at[c], "tp", near)

    far_copies = [far_copy(c) for c in range(CHUNKS)]
    forwards = [forward(c) for c in range(CHUNKS)]
    near_copy = remote(held.at[me], held.at[me], near_sem.at[0], near_sem.at[1], "tp", near)
    for copy in far_copies:
        copy.start()
    near_copy.start()

    def project(slot):
        block = held[slot]
        at = pl.ds(pl.multiple_of(slot * rows, rows), rows)
        for i in range(6):
            res = jnp.dot(block, wbuf[i], preferred_element_type=jnp.float32).astype(jnp.bfloat16)
            if i < 2:
                wide = res.astype(jnp.float32)
                wide = wide * group_scale(wide, comp) * qk_ref[i : i + 1]
                res = wide.astype(jnp.bfloat16)
            if i == 0:
                q_ref[at, :] = res
            elif i < 3:
                kv_ref[at, (i - 1) * wcols : i * wcols] = res
            else:
                conv_ref[at, (i - 3) * wcols : (i - 2) * wcols] = res

    for load in loads:
        load.wait()
    project(me)
    near_copy.wait_recv()
    project(near)
    for c in range(CHUNKS):
        far_copies[c].wait_recv()
        forwards[c].start()
    project(far)
    for copy in forwards:
        copy.wait_recv()
    project(diag)
    near_copy.wait_send()
    for copy in far_copies + forwards:
        copy.wait_send()


def attend(
    heads, q_ref, kv_ref, lam_ref, sub_ref, proj_ref, taps_ref, cgain_ref, out_ref, log_ref,
    conv_ref, buf, qpad, top, total, acc, tail, padded, up_send, side_send, recv, tail_sem,
):
    n = buf.shape[0]
    me = lax.axis_index("sp")
    z, x = me // 2, lax.rem(me, 2)
    levels = n // 2
    partner = z * 2 + 1 - x
    rows = q_ref.shape[0]
    both = q_ref.shape[1] // heads
    comp = both // 2
    vsize = sub_ref.shape[0]
    barrier = pltpu.get_barrier_semaphore()
    has_up, has_down = z < levels - 1, z > 0
    pl.semaphore_signal(barrier, inc=1, device_id={"sp": partner}, device_id_type=MESH)

    @pl.when(has_up)
    def _():
        pl.semaphore_signal(barrier, inc=1, device_id={"sp": me + 2}, device_id_type=MESH)

    @pl.when(has_down)
    def _():
        pl.semaphore_signal(barrier, inc=1, device_id={"sp": me - 2}, device_id_type=MESH)

    ups, downs = has_up.astype(jnp.int32), has_down.astype(jnp.int32)

    @pl.when((x == 1) & has_up)
    def _():
        pl.semaphore_signal(barrier, inc=1, device_id={"sp": me + 1}, device_id_type=MESH)

    @pl.when((x == 0) & has_down)
    def _():
        pl.semaphore_signal(barrier, inc=1, device_id={"sp": me - 1}, device_id_type=MESH)

    pl.semaphore_wait(barrier, 1 + ups + downs + x * ups + (1 - x) * downs)
    edge = tail.shape[0]
    channels = conv_ref.shape[1]
    tail_copy = remote(
        proj_ref.at[pl.ds(rows - edge, edge), pl.ds(channels, 2 * channels)], tail,
        tail_sem.at[0], tail_sem.at[1], "sp", jnp.minimum(me + 1, n - 1),
    )
    size = rows // HALVES

    def up_copy(src, block, half):
        at = pl.ds(half * size, size)
        return remote(
            src.at[at], buf.at[block, at], up_send.at[block // 2, half], recv.at[block, half],
            "sp", jnp.minimum(me + 2, n - 2 + x),
        )

    def side_copy(src, block, half):
        at = pl.ds(half * size, size)
        return remote(
            src.at[at], buf.at[block, at], side_send.at[block // 2, half], recv.at[block, half],
            "sp", partner,
        )

    @pl.when(has_up)
    def _():
        for half in range(HALVES):
            up_copy(kv_ref, me, half).start()

    @pl.when(x == 0)
    def _():
        for half in range(HALVES):
            side_copy(kv_ref, me, half).start()

    @pl.when(me < n - 1)
    def _():
        tail_copy.start()

    lane = lax.broadcasted_iota(jnp.int32, (rows, both), 1)
    for h in range(heads):
        q = q_ref[:, h * both : (h + 1) * both]
        zero = jnp.zeros_like(q)
        qpad[h, :rows] = jnp.where(lane < comp, q, zero)
        qpad[h, rows:] = jnp.where(lane < comp, zero, q)
    top[...] = jnp.full_like(top, -1e30)
    total[...] = jnp.zeros_like(total)
    acc[...] = jnp.zeros_like(acc)
    tile = min(256, rows)

    def absorb(piece, masked):
        for h in range(heads):
            for start in range(0, 2 * rows, tile):
                first = start % rows
                keys = first + tile if masked else rows
                k = piece[:keys, h * both : (h + 1) * both]
                v = piece[:keys, heads * both + h * vsize : heads * both + (h + 1) * vsize]
                at = slice(start, start + tile)
                s = lax.dot_general(
                    k, qpad[h, at], (((1,), (1,)), ((), ())), preferred_element_type=jnp.float32
                )
                if masked:
                    kpos = lax.broadcasted_iota(jnp.int32, s.shape, 0)
                    qpos = first + lax.broadcasted_iota(jnp.int32, s.shape, 1)
                    s = jnp.where(kpos <= qpos, s, -1e30)
                old = top[h : h + 1, at]
                new = jnp.maximum(old, jnp.max(s, axis=0, keepdims=True))
                p = jnp.exp(s - new)
                factor = jnp.exp(old - new)
                top[h : h + 1, at] = new
                total[h : h + 1, at] = total[h : h + 1, at] * factor + jnp.sum(
                    p, axis=0, keepdims=True
                )
                acc[h, :, at] = acc[h, :, at] * factor + lax.dot_general(
                    v, p.astype(jnp.bfloat16), (((0,), (0,)), ((), ())),
                    preferred_element_type=jnp.float32,
                )

    absorb(kv_ref, True)

    def product(ref, at):
        gate = ref[:, at : at + channels].astype(jnp.float32)
        other = ref[:, at + channels : at + 2 * channels].astype(jnp.float32)
        return (gate * other).astype(jnp.bfloat16).astype(jnp.float32)

    padded[edge:] = product(proj_ref, channels)

    @pl.when(me > 0)
    def _():
        tail_copy.wait_recv()
        padded[:edge] = product(tail, 0)

    @pl.when(me == 0)
    def _():
        padded[:edge] = jnp.zeros((edge, channels), jnp.float32)

    count = taps_ref.shape[0]
    conv = jnp.zeros((rows, channels), jnp.float32)
    for tap in range(count):
        first = edge - count + 1 + tap
        conv = conv + taps_ref[tap : tap + 1] * padded[first : first + rows]
    gated = proj_ref[:, :channels].astype(jnp.float32) * conv
    conv_ref[...] = (gated * group_scale(gated, GROUP) * cgain_ref[...]).astype(jnp.bfloat16)

    @pl.loop(0, 2 * (z + 1))
    def _(j):
        step, other = j // 2 + 1, lax.rem(j, 2)
        level = z - step + other
        block = jnp.maximum(level, 0) * 2 + x + other * (1 - 2 * x)
        valid = jnp.where(other == 0, step <= z, (x == 1) | (step >= 2))

        @pl.when(valid)
        def _():
            for half in range(HALVES):
                side_copy(buf.at[block], block, half).wait_recv()

                @pl.when(other == 0)
                def _():
                    @pl.when(has_up)
                    def _():
                        up_copy(buf.at[block], block, half).start()

                    side_copy(buf.at[block], block, half).start()

            absorb(buf.at[block], False)

    for h in range(heads):
        mapped = acc[h] / total[h : h + 1]
        attn = mapped[:, :rows] - lam_ref[h] * mapped[:, rows:]
        scale = lax.rsqrt(jnp.mean(attn * attn, axis=0, keepdims=True) + eps)
        result = attn * scale * sub_ref[...]
        out_ref[:, h * vsize : (h + 1) * vsize] = result.T.astype(jnp.bfloat16)
        logs = top[h : h + 1] + jnp.log(total[h : h + 1])
        log_ref[h, 0:1, :] = logs[:, :rows]
        log_ref[h, 1:2, :] = logs[:, rows:]

    @pl.loop(0, z + 1)
    def _(level):
        block = level * 2 + x

        @pl.when(has_up)
        def _():
            for half in range(HALVES):
                up_copy(kv_ref, block, half).wait_send()

        @pl.when((x == 0) | (level < z))
        def _():
            for half in range(HALVES):
                side_copy(kv_ref, block, half).wait_send()

    @pl.when(me < n - 1)
    def _():
        tail_copy.wait_send()


def project_scatter(
    heads_ref, conv_ref, wa_ref, wc_ref, out_ref, cross, fin, far, cross_in, fin_in, far_in,
    cross_send, cross_recv, fin_send, fin_recv, far_send, far_recv,
):
    me = lax.axis_index("tp")
    near, other = flip(me, 1), flip(me, 2)
    diag = flip(near, 2)
    rows = out_ref.shape[0]
    width = out_ref.shape[1] // CHUNKS
    greet("tp", (near, other))

    def partial(target, c):
        at = pl.ds(pl.multiple_of(target * rows, rows), rows)
        cols = slice(c * width, (c + 1) * width)
        return jnp.dot(
            heads_ref[at, :], wa_ref[:, cols], preferred_element_type=jnp.float32
        ) + jnp.dot(conv_ref[at, :], wc_ref[:, cols], preferred_element_type=jnp.float32)

    crosses = [
        remote(cross.at[c], cross_in.at[c], cross_send.at[c], cross_recv.at[c], "tp", near)
        for c in range(CHUNKS)
    ]
    fins = [
        remote(fin.at[c], fin_in.at[c], fin_send.at[c], fin_recv.at[c], "tp", near)
        for c in range(CHUNKS)
    ]
    fars = [
        remote(far.at[c], far_in.at[c], far_send.at[c], far_recv.at[c], "tp", other)
        for c in range(CHUNKS)
    ]
    for c in range(CHUNKS):
        cross[c] = partial(diag, c).astype(jnp.bfloat16)
        crosses[c].start()
    for c in range(CHUNKS):
        mine = partial(other, c)
        crosses[c].wait_recv()
        far[c] = (mine + cross_in[c].astype(jnp.float32)).astype(jnp.bfloat16)
        fars[c].start()
    for c in range(CHUNKS):
        fin[c] = partial(near, c).astype(jnp.bfloat16)
        fins[c].start()
    for c in range(CHUNKS):
        cols = slice(c * width, (c + 1) * width)
        out_ref[:, cols] = partial(me, c)
    for c in range(CHUNKS):
        cols = slice(c * width, (c + 1) * width)
        fins[c].wait_recv()
        fars[c].wait_recv()
        out_ref[:, cols] += fin_in[c].astype(jnp.float32) + far_in[c].astype(jnp.float32)
    for copy in crosses + fins + fars:
        copy.wait_send()


def vmem():
    return pl.BlockSpec(memory_space=pltpu.VMEM)


def on_device(
    inputs, norm_gain, w_query, w_key, w_value, query_gain, key_gain, lambdas, sub_gain,
    w_gate_b, w_gate_c, w_conv_in, conv_taps, conv_gain, w_out_att, w_out_conv,
):
    heads = lambdas.shape[0]
    comp = query_gain.shape[1]
    vsize = sub_gain.shape[0]
    channels = conv_gain.shape[0]
    own, width = inputs.shape
    tp = lax.axis_size("tp")
    sp = lax.axis_size("sp")
    rows = own * tp
    dma = pltpu.SemaphoreType.DMA

    def params(cid):
        return pltpu.CompilerParams(
            collective_id=cid, has_side_effects=True, vmem_limit_bytes=VMEM_LIMIT
        )

    qcols = heads * 2 * comp
    weights = (w_query, w_key, w_value, w_gate_b, w_gate_c, w_conv_in)
    qk_gain = jnp.stack(
        [
            jnp.tile(query_gain.reshape(-1) * comp ** (-0.5), heads),
            jnp.tile(key_gain.reshape(-1), heads),
        ]
    )
    qn, kv, conv_proj = pl.pallas_call(
        functools.partial(gather_project, comp),
        out_shape=(
            jax.ShapeDtypeStruct((rows, qcols), jnp.bfloat16),
            jax.ShapeDtypeStruct((rows, 2 * qcols), jnp.bfloat16),
            jax.ShapeDtypeStruct((rows, 3 * channels), jnp.bfloat16),
        ),
        in_specs=[vmem()] * 3 + [pl.BlockSpec(memory_space=pl.ANY)] * 6,
        out_specs=(vmem(), vmem(), vmem()),
        scratch_shapes=[
            pltpu.VMEM((tp, own, width), jnp.bfloat16),
            pltpu.VMEM((6, width, qcols), jnp.bfloat16),
            dma((6,)), dma((CHUNKS,)), dma((CHUNKS,)), dma((2,)), dma((CHUNKS,)), dma((CHUNKS,)),
        ],
        compiler_params=params(0),
        name="gather_project",
    )(inputs, norm_gain[None], qk_gain, *weights)

    heads_out, log_sums, conv_out = pl.pallas_call(
        functools.partial(attend, heads),
        out_shape=(
            jax.ShapeDtypeStruct((rows, heads * vsize), jnp.bfloat16),
            jax.ShapeDtypeStruct((heads, 2, rows), jnp.float32),
            jax.ShapeDtypeStruct((rows, channels), jnp.bfloat16),
        ),
        in_specs=[vmem(), vmem(), pl.BlockSpec(memory_space=pltpu.SMEM)] + [vmem()] * 4,
        out_specs=(vmem(), vmem(), vmem()),
        scratch_shapes=[
            pltpu.VMEM((sp, rows, kv.shape[1]), jnp.bfloat16),
            pltpu.VMEM((heads, 2 * rows, 2 * comp), jnp.bfloat16),
            pltpu.VMEM((heads, 2 * rows), jnp.float32),
            pltpu.VMEM((heads, 2 * rows), jnp.float32),
            pltpu.VMEM((heads, vsize, 2 * rows), jnp.float32),
            pltpu.VMEM((16, 2 * channels), jnp.bfloat16),
            pltpu.VMEM((16 + rows, channels), jnp.float32),
            dma((sp // 2, HALVES)), dma((sp // 2, HALVES)), dma((sp, HALVES)), dma((2,)),
        ],
        compiler_params=params(1),
        cost_estimate=pl.CostEstimate(flops=20_000_000_000, bytes_accessed=0, transcendentals=0),
        name="attend",
    )(qn, kv, lambdas, sub_gain[:, None], conv_proj, conv_taps, conv_gain[None])

    piece = pltpu.VMEM((CHUNKS, own, width // CHUNKS), jnp.bfloat16)
    mixed = pl.pallas_call(
        project_scatter,
        out_shape=jax.ShapeDtypeStruct((own, width), jnp.float32),
        in_specs=[vmem()] * 4,
        out_specs=vmem(),
        scratch_shapes=[piece] * 6 + [dma((CHUNKS,))] * 6,
        compiler_params=params(2),
        name="project_scatter",
    )(heads_out, conv_out, w_out_att, w_out_conv)
    return (mixed, log_sums)


def solution(mesh):
    in_specs = (
        P(("sp", "tp"), None),
        P(),
        P(None, "tp"),
        P(None, "tp"),
        P(None, "tp"),
        P(),
        P(),
        P("tp"),
        P(),
        P(None, "tp"),
        P(None, "tp"),
        P(None, "tp"),
        P(None, "tp"),
        P("tp"),
        P("tp", None),
        P("tp", None),
    )
    out_specs = (P(("sp", "tp"), None), P("tp", None, "sp"))
    return jax.shard_map(
        on_device, mesh=mesh, in_specs=in_specs, out_specs=out_specs, check_vma=False
    )
```
